32 devices in a mesh: sp: 8 (over z, y), dp: 4 (over x, core).
Axes of the slice: x: 2, y: 2, z: 4, core: 2. Of those that a mesh axis runs over, the one named last changes fastest.
Arguments:
- tokens: bfloat16 [4, 2048, 2048], P('dp', 'sp'), may hold values from -6 to 6
- in_gain: float32 [2048], replicated, may hold values from 0.1 to 1.9
- w_query_down: bfloat16 [2048, 512], P('dp'), may hold values from -0.125 to 0.125
- w_latent_down: bfloat16 [2048, 256], P('dp'), may hold values from -0.125 to 0.125
- w_rope_key: bfloat16 [2048, 64], replicated, may hold values from -0.125 to 0.125
- query_latent_gain: float32 [512], replicated, may hold values from 0.1 to 1.9
- latent_gain: float32 [256], replicated, may hold values from 0.1 to 1.9
- w_query_up: bfloat16 [512, 3072], P('dp', 'sp'), may hold values from -0.25 to 0.25
- w_key_up: bfloat16 [256, 2048], P('dp', 'sp'), may hold values from -0.375 to 0.375
- w_value_up: bfloat16 [256, 2048], P('dp', 'sp'), may hold values from -0.375 to 0.375
- query_gain: float32 [192], replicated, may hold values from 0.5 to 14
- key_gain: float32 [192], replicated, may hold values from 0.5 to 14
- out_gain: float32 [2048], replicated, may hold values from 0.1 to 1.9
- w_out: bfloat16 [2048, 2048], P(('sp', 'dp')), may hold values from -0.125 to 0.125
Outputs:
- result: bfloat16 [4, 2048, 2048], P('dp', 'sp')
The draws below stay inside these ranges and needn't reach their ends.
All inputs are finite; a program needn't handle non-finite values.
Results may differ from the reference program's by a relative error of at most 0.034.
The reference program's roundings to bfloat16 on the way count: a program that leaves them out, or rounds other values in their place, can miss the bound.
Values may be sent and summed in bfloat16 or wider, within the bound.
A program may use at most 64 MiB of HBM per device.

```python
import jax
import jax.numpy as jnp
from jax import lax

D = 2048
HEADS = 16
NOPE = 128
ROPE = 64
VD = 128
QR = 512
KR = 256
QK = 192
LEN = 2048
SEQS = 4


def gain_vector(key, member):
    spread = jnp.clip(jax.random.normal(jax.random.fold_in(key, 11 + member), (QK,), jnp.float32), -2.5, 2.5)
    return (1.0 + 0.18 * spread).astype(jnp.float32)


def draw_query_gain(key, part):
    return gain_vector(key, 0)


def draw_key_gain(key, part):
    return gain_vector(key, 1)


def block_levels(own_key, shape, split, least, largest):
    gain, own = 1.0, jax.random.fold_in(own_key, 6)
    for dim, parts in split:
        draws = jnp.exp(jax.random.uniform(jax.random.fold_in(own, dim), (parts,), jnp.float32, least / len(split), largest / len(split)))
        gain = gain * jnp.repeat(draws, shape[dim] // parts).reshape([-1 if axis == dim else 1 for axis in range(len(shape))])
    return gain


def centred(stream_key, shape, scale, limit, split=(), kind=jnp.bfloat16):
    values = jax.random.normal(stream_key, shape, jnp.float32) * scale
    if len(split) > 0:
        values = block_levels(stream_key, shape, split, -0.22, 0.18) * values
    return jnp.clip(values, min=-limit, max=limit).astype(kind)


def setup_inputs(seed: int = 0) -> dict:
    arg_keys = jax.random.split(jax.random.key(seed), 15)
    tokens = centred(arg_keys[0], (SEQS, LEN, D), 1.0, 6.0, ((0, 4), (1, 8)))
    in_gain = jnp.clip(1.0 + 0.18 * jax.random.normal(arg_keys[1], (D,), jnp.float32), 0.1, 1.9)
    w_query_down = centred(arg_keys[2], (D, QR), D ** -0.5, 0.125, ((0, 4),))
    w_latent_down = centred(arg_keys[3], (D, KR), D ** -0.5, 0.125, ((0, 4),))
    w_rope_key = centred(arg_keys[4], (D, ROPE), D ** -0.5, 0.125)
    query_latent_gain = jnp.clip(1.0 + 0.18 * jax.random.normal(arg_keys[5], (QR,), jnp.float32), 0.1, 1.9)
    latent_gain = jnp.clip(1.0 + 0.18 * jax.random.normal(arg_keys[6], (KR,), jnp.float32), 0.1, 1.9)
    w_query_up = centred(arg_keys[7], (QR, HEADS * QK), QR ** -0.5, 0.25, ((0, 4), (1, 8)))
    w_key_up = centred(arg_keys[8], (KR, HEADS * NOPE), KR ** -0.5, 0.375, ((0, 4), (1, 8)))
    w_value_up = centred(arg_keys[9], (KR, HEADS * VD), KR ** -0.5, 0.375, ((0, 4), (1, 8)))
    query_gain = draw_query_gain(jax.random.fold_in(arg_keys[14], 71), 0)
    key_gain = draw_key_gain(jax.random.fold_in(arg_keys[14], 71), 0)
    out_gain = jnp.clip(1.0 + 0.18 * jax.random.normal(arg_keys[12], (HEADS * VD,), jnp.float32), 0.1, 1.9)
    w_out = centred(arg_keys[13], (HEADS * VD, D), (HEADS * VD) ** -0.5, 0.125, ((0, 32),))
    return dict(tokens=tokens, in_gain=in_gain, w_query_down=w_query_down, w_latent_down=w_latent_down, w_rope_key=w_rope_key, query_latent_gain=query_latent_gain, latent_gain=latent_gain, w_query_up=w_query_up, w_key_up=w_key_up, w_value_up=w_value_up, query_gain=query_gain, key_gain=key_gain, out_gain=out_gain, w_out=w_out)


EPS = 1e-06
THETA = 10000.0
NEG_BIG = -1e+30

def rms_scale(values, scaling):
    return values * lax.rsqrt(lax.optimization_barrier(jnp.mean(values * values, axis=-1, keepdims=True)) + EPS) * scaling

def rotate(tail_part, positions):
    half_width = tail_part.shape[-1] // 2
    frequency = THETA ** (-jnp.arange(half_width, dtype=jnp.float32) / half_width)
    angles = positions[:, None] * frequency[None, :]
    cosine = jnp.cos(angles)[:, None, :]
    sine = jnp.sin(angles)[:, None, :]
    first_half = tail_part[..., :half_width]
    second_half = tail_part[..., half_width:]
    return jnp.concatenate([first_half * cosine - second_half * sine, second_half * cosine + first_half * sine], axis=-1)

def finish_heads(joined, positions, scaling, rope_width):
    row_count = joined.shape[0]
    normal = rms_scale(joined, scaling)
    turned = rotate(normal[..., -rope_width:], positions)
    return jnp.concatenate([normal[..., :-rope_width], turned], axis=-1).astype(jnp.bfloat16).reshape(row_count, -1)

def attend(queries, keys, values, head_count):
    length = queries.shape[0]
    block_rows = min(512, length)
    query_blocks = queries.reshape(length // block_rows, block_rows, head_count, -1)
    key_heads = keys.reshape(length, head_count, -1).astype(jnp.float32)
    value_heads = values.reshape(length, head_count, -1).astype(jnp.float32)
    score_scale = key_heads.shape[-1] ** (-0.5)
    key_pos = jnp.arange(length)

    def one_block(block_args):
        query_block, block_index = block_args
        scores = jnp.einsum('qhd,khd->hqk', query_block.astype(jnp.float32), key_heads) * score_scale
        query_pos = block_index * block_rows + jnp.arange(block_rows)
        allowed = key_pos[None, :] <= query_pos[:, None]
        scores = jnp.where(allowed[None], scores, NEG_BIG)
        weights = jax.nn.softmax(scores, axis=-1).astype(jnp.bfloat16)
        return jnp.einsum('hqk,khd->qhd', weights.astype(jnp.float32), value_heads).astype(jnp.bfloat16)
    outcome = lax.map(one_block, (query_blocks, jnp.arange(length // block_rows)))
    return outcome.reshape(length, -1)

def reference(tokens, in_gain, w_query_down, w_latent_down, w_rope_key, query_latent_gain, latent_gain, w_query_up, w_key_up, w_value_up, query_gain, key_gain, out_gain, w_out):

    def one_sequence(sequence):
        normed = rms_scale(sequence.astype(jnp.float32), in_gain).astype(jnp.bfloat16)
        latent_q = rms_scale(jnp.dot(normed, w_query_down, preferred_element_type=jnp.float32), query_latent_gain).astype(jnp.bfloat16)
        latent_kv = rms_scale(jnp.dot(normed, w_latent_down, preferred_element_type=jnp.float32), latent_gain).astype(jnp.bfloat16)
        rope_key = jnp.dot(normed, w_rope_key, preferred_element_type=jnp.float32).astype(jnp.bfloat16)
        positions = jnp.arange(LEN, dtype=jnp.float32)
        query_total = jnp.dot(latent_q, w_query_up, preferred_element_type=jnp.float32)
        queries = finish_heads(query_total.reshape(LEN, HEADS, QK), positions, query_gain, ROPE)
        key_total = jnp.dot(latent_kv, w_key_up, preferred_element_type=jnp.float32).reshape(LEN, HEADS, NOPE)
        shared = jnp.broadcast_to(rope_key.astype(jnp.float32)[:, None, :], (LEN, HEADS, ROPE))
        keys = finish_heads(jnp.concatenate([key_total, shared], axis=-1), positions, key_gain, ROPE)
        values = jnp.dot(latent_kv, w_value_up, preferred_element_type=jnp.float32).astype(jnp.bfloat16)
        attended = attend(queries, keys, values, HEADS)
        mixed = rms_scale(attended.astype(jnp.float32), out_gain).astype(jnp.bfloat16)
        return jnp.dot(mixed, w_out, preferred_element_type=jnp.float32).astype(jnp.bfloat16)
    return lax.map(one_sequence, tokens)
```

```python
import functools

import jax
import jax.numpy as jnp
from jax import lax
from jax.experimental import pallas as pl
from jax.experimental.pallas import tpu as pltpu
from jax.sharding import PartitionSpec as P

HEADS = 16
EPS = 1e-06
THETA = 10000.0
NEG_BIG = -1e30
LOG2E = 1.4426950408889634
NT = (((1,), (1,)), ((), ()))


def rms_scale(values, scaling):
    return values * lax.rsqrt(jnp.mean(values * values, axis=-1, keepdims=True) + EPS) * scaling


def swap_halves(x):
    half = x.shape[-1] // 2
    return jnp.concatenate([x[..., half:], x[..., :half]], axis=-1)


def tables(length, width, gains):
    half = width // 2
    frequency = THETA ** (-jnp.arange(half, dtype=jnp.float32) / half)
    angles = jnp.arange(length, dtype=jnp.float32)[:, None] * frequency[None, :]
    cosine, sine = jnp.cos(angles), jnp.sin(angles)
    base = jnp.concatenate([cosine, cosine, -sine, sine], axis=-1)
    out = []
    for gain in gains:
        tail = gain[-width:]
        out.append(base * jnp.concatenate([tail, swap_halves(tail)])[None, :])
    return out


def widen_query(w, head_count, rope):
    rows = w.shape[0]
    w = w.reshape(rows, head_count, -1)
    return jnp.concatenate([w, swap_halves(w[..., -rope:])], axis=-1).reshape(rows, -1)


def project_block(i, rows, heads, nope, vd, lq, lkv, rp, wq, wk, wvt, gq, gk, tq, tk, q_s, k_s, v_s):
    tok = pl.ds(pl.multiple_of(i * rows, rows), rows)
    wide = wq.shape[1] // heads
    rope2 = wide - nope
    inv = 1.0 / (nope + rope2 // 2)
    q = jnp.dot(lq, wq[...], preferred_element_type=jnp.float32)
    k = jnp.dot(lkv, wk[...], preferred_element_type=jnp.float32)
    v_s[:, tok] = lax.dot_general(wvt[...], lkv, NT, preferred_element_type=jnp.float32).astype(jnp.bfloat16)
    shared = rp.astype(jnp.float32)
    shared_sq = 0.5 * shared * shared
    lane = lax.broadcasted_iota(jnp.int32, (rows, rope2), 1)
    tqv, tkv = tq[tok, :], tk[tok, :]
    for h in range(heads):
        for which in range(2):
            if which == 0:
                t1 = q[:, h * wide : h * wide + nope]
                t2 = q[:, h * wide + nope : (h + 1) * wide]
                sq, gain, table, dest = t1 * t1 + 0.5 * t2 * t2, gq, tqv, q_s
            else:
                t1, t2 = k[:, h * nope : (h + 1) * nope], shared
                sq, gain, table, dest = t1 * t1 + shared_sq, gk, tkv, k_s
            r = lax.rsqrt(jnp.sum(sq, axis=-1, keepdims=True) * inv + EPS)
            dest[h, tok, 0:nope] = (t1 * r * gain[...]).astype(jnp.bfloat16)
            y = t2 * r * table
            y = y + pltpu.roll(y, rope2 // 2, 1)
            if which == 1:
                y = jnp.where(lane < rope2 // 2, y, 0.0)
            dest[h, tok, nope:wide] = y.astype(jnp.bfloat16)


def attend_block(qb, rows, chunk, heads, vd, scale, q_s, k_s, v_s):
    qtok = pl.ds(pl.multiple_of(qb * rows, rows), rows)
    qs = [q_s[h, qtok, :] for h in range(heads)]
    factor = scale * LOG2E

    def step(kb, carry, masked):
        ktok = pl.ds(pl.multiple_of(kb * chunk, chunk), chunk)
        new = []
        for h in range(heads):
            m, l, acc = carry[h]
            s = lax.dot_general(k_s[h, ktok, :], qs[h], NT, preferred_element_type=jnp.float32) * factor
            if masked:
                kpos = kb * chunk + lax.broadcasted_iota(jnp.int32, (chunk, rows), 0)
                qpos = qb * rows + lax.broadcasted_iota(jnp.int32, (chunk, rows), 1)
                s = jnp.where(kpos <= qpos, s, NEG_BIG)
            m_new = jnp.maximum(m, jnp.max(s, axis=0, keepdims=True))
            alpha = jnp.exp2(m - m_new)
            p = jnp.exp2(s - m_new)
            l = l * alpha + jnp.sum(p, axis=0, keepdims=True)
            vt = v_s[h * vd : (h + 1) * vd, ktok]
            acc = acc * alpha + jnp.dot(vt, p.astype(jnp.bfloat16), preferred_element_type=jnp.float32)
            new.append((m_new, l, acc))
        return tuple(new)

    carry = tuple(
        (
            jnp.full((1, rows), NEG_BIG, jnp.float32),
            jnp.zeros((1, rows), jnp.float32),
            jnp.zeros((vd, rows), jnp.float32),
        )
        for _ in range(heads)
    )
    last = (qb * rows) // chunk
    carry = lax.fori_loop(0, last, lambda kb, c: step(kb, c, False), carry)
    carry = step(last, carry, True)
    return jnp.concatenate([jnp.transpose(acc / l) for _, l, acc in carry], axis=1).astype(jnp.bfloat16)


def attention_kernel(
    blocks, rows, chunk, heads, nope, vd, scale,
    lq, lkv, rp, wq, wk, wvt, gq, gk, tq, tk, out, q_s, k_s, v_s,
):
    def project(i, _):
        tok = pl.ds(pl.multiple_of(i * rows, rows), rows)
        project_block(
            i, rows, heads, nope, vd, lq[tok, :], lkv[tok, :], rp[tok, :],
            wq, wk, wvt, gq, gk, tq, tk, q_s, k_s, v_s,
        )
        return 0

    lax.fori_loop(0, blocks, project, 0)

    def attend(qb, _):
        tok = pl.ds(pl.multiple_of(qb * rows, rows), rows)
        out[tok, :] = attend_block(qb, rows, chunk, heads, vd, scale, q_s, k_s, v_s)
        return 0

    lax.fori_loop(0, blocks, attend, 0)


def per_device(
    tokens, in_gain, w_query_down, w_latent_down, w_rope_key, query_latent_gain, latent_gain,
    w_query_up, w_key_up, w_value_up, query_gain, key_gain, out_gain, w_out,
):
    seq_devices = lax.axis_size("sp")
    heads = HEADS // seq_devices
    own_rows = tokens.shape[1]
    length = own_rows * seq_devices
    rope = w_rope_key.shape[1]
    nope = w_key_up.shape[1] // heads
    vd = w_value_up.shape[1] // heads
    qk = nope + rope
    qr, kr = w_query_down.shape[1], w_latent_down.shape[1]
    out_full = lax.all_gather(w_out, ("sp", "dp"), axis=0, tiled=True)
    local_rows = tokens.reshape(own_rows, tokens.shape[2])
    normed = rms_scale(local_rows.astype(jnp.float32), in_gain).astype(jnp.bfloat16)
    down = lax.all_gather(
        jnp.concatenate([w_query_down, w_latent_down], axis=1), "dp", axis=0, tiled=True
    )
    sums = jnp.dot(normed, down, preferred_element_type=jnp.float32)
    latent_q = rms_scale(sums[:, :qr], query_latent_gain).astype(jnp.bfloat16)
    latent_kv = rms_scale(sums[:, qr:], latent_gain).astype(jnp.bfloat16)
    wide_rope = jnp.concatenate([w_rope_key, swap_halves(w_rope_key)], axis=1)
    rope_key = jnp.dot(normed, wide_rope, preferred_element_type=jnp.float32).astype(jnp.bfloat16)
    lat = lax.all_gather(
        jnp.concatenate([latent_q, latent_kv, rope_key], axis=1), "sp", axis=0, tiled=True
    )
    wq = lax.all_gather(w_query_up, "dp", axis=0, tiled=True)
    wkv = lax.all_gather(jnp.concatenate([w_key_up, w_value_up], axis=1), "dp", axis=0, tiled=True)
    wk, wv = wkv[:, : heads * nope], wkv[:, heads * nope :]
    tq, tk = tables(length, rope, (query_gain, key_gain))
    chunk = min(2 * own_rows, length)
    attended = pl.pallas_call(
        functools.partial(
            attention_kernel, seq_devices, own_rows, chunk, heads, nope, vd, float(qk) ** -0.5
        ),
        out_shape=jax.ShapeDtypeStruct((length, heads * vd), jnp.bfloat16),
        scratch_shapes=[
            pltpu.VMEM((heads, length, qk + rope), jnp.bfloat16),
            pltpu.VMEM((heads, length, qk + rope), jnp.bfloat16),
            pltpu.VMEM((heads * vd, length), jnp.bfloat16),
        ],
        compiler_params=pltpu.CompilerParams(vmem_limit_bytes=56 * 1024 * 1024),
        cost_estimate=pl.CostEstimate(flops=8 * 10**9, bytes_accessed=10**7, transcendentals=5 * 10**6),
    )(
        lat[:, :qr], lat[:, qr : qr + kr], lat[:, qr + kr :],
        widen_query(wq, heads, rope), wk, wv.T,
        query_gain[None, :nope], key_gain[None, :nope], tq, tk,
    )
    token_heads = lax.all_to_all(attended, "sp", split_axis=0, concat_axis=1, tiled=True)
    mixed = rms_scale(token_heads.astype(jnp.float32), out_gain).astype(jnp.bfloat16)
    projected = jnp.dot(mixed, out_full, preferred_element_type=jnp.float32)
    return projected.astype(jnp.bfloat16).reshape(1, own_rows, w_out.shape[1])


def solution(mesh):
    in_specs = (
        P("dp", "sp", None), P(), P("dp", None), P("dp", None), P(), P(), P(),
        P("dp", "sp"), P("dp", "sp"), P("dp", "sp"), P(), P(), P(), P(("sp", "dp"), None),
    )
    return jax.shard_map(
        per_device, mesh=mesh, in_specs=in_specs, out_specs=P("dp", "sp", None), check_vma=False
    )
```

```python
import functools

import jax
import jax.numpy as jnp
from jax import lax
from jax.experimental import pallas as pl
from jax.experimental.pallas import tpu as pltpu
from jax.sharding import PartitionSpec as P

HEADS = 16
EPS = 1e-06
THETA = 10000.0
NEG_BIG = -1e30
LOG2E = 1.4426950408889634
NT = (((1,), (1,)), ((), ()))


def rms_scale(values, scaling):
    return values * lax.rsqrt(jnp.mean(values * values, axis=-1, keepdims=True) + EPS) * scaling


def swap_halves(x):
    half = x.shape[-1] // 2
    return jnp.concatenate([x[..., half:], x[..., :half]], axis=-1)


def tables(length, width, gains):
    half = width // 2
    frequency = THETA ** (-jnp.arange(half, dtype=jnp.float32) / half)
    angles = jnp.arange(length, dtype=jnp.float32)[:, None] * frequency[None, :]
    cosine, sine = jnp.cos(angles), jnp.sin(angles)
    base = jnp.concatenate([cosine, cosine, -sine, sine], axis=-1)
    out = []
    for gain in gains:
        tail = gain[-width:]
        out.append(base * jnp.concatenate([tail, swap_halves(tail)])[None, :])
    return out


def widen_query(w, head_count, rope):
    rows = w.shape[0]
    w = w.reshape(rows, head_count, -1)
    return jnp.concatenate([w, swap_halves(w[..., -rope:])], axis=-1).reshape(rows, -1)


def project_block(i, rows, heads, nope, vd, lq, lkv, rp, wq, wk, wvt, gq, gk, tq, tk, q_s, k_s, v_s):
    tok = pl.ds(pl.multiple_of(i * rows, rows), rows)
    wide = wq.shape[1] // heads
    rope2 = wide - nope
    inv = 1.0 / (nope + rope2 // 2)
    q = jnp.dot(lq, wq[...], preferred_element_type=jnp.float32)
    k = jnp.dot(lkv, wk[...], preferred_element_type=jnp.float32)
    v_s[:, tok] = lax.dot_general(wvt[...], lkv, NT, preferred_element_type=jnp.float32).astype(jnp.bfloat16)
    shared = rp.astype(jnp.float32)
    shared_sq = 0.5 * shared * shared
    lane = lax.broadcasted_iota(jnp.int32, (rows, rope2), 1)
    tqv, tkv = tq[tok, :], tk[tok, :]
    for h in range(heads):
        for which in range(2):
            if which == 0:
                t1 = q[:, h * wide : h * wide + nope]
                t2 = q[:, h * wide + nope : (h + 1) * wide]
                sq, gain, table, dest = t1 * t1 + 0.5 * t2 * t2, gq, tqv, q_s
            else:
                t1, t2 = k[:, h * nope : (h + 1) * nope], shared
                sq, gain, table, dest = t1 * t1 + shared_sq, gk, tkv, k_s
            r = lax.rsqrt(jnp.sum(sq, axis=-1, keepdims=True) * inv + EPS)
            dest[h, tok, 0:nope] = (t1 * r * gain[...]).astype(jnp.bfloat16)
            y = t2 * r * table
            y = y + pltpu.roll(y, rope2 // 2, 1)
            if which == 1:
                y = jnp.where(lane < rope2 // 2, y, 0.0)
            dest[h, tok, nope:wide] = y.astype(jnp.bfloat16)


def attend_block(qb, rows, chunk, heads, vd, scale, q_s, k_s, v_s):
    qtok = pl.ds(pl.multiple_of(qb * rows, rows), rows)
    qs = [q_s[h, qtok, :] for h in range(heads)]
    factor = scale * LOG2E

    def step(kb, carry, masked):
        ktok = pl.ds(pl.multiple_of(kb * chunk, chunk), chunk)
        new = []
        for h in range(heads):
            m, l, acc = carry[h]
            s = lax.dot_general(k_s[h, ktok, :], qs[h], NT, preferred_element_type=jnp.float32) * factor
            if masked:
                kpos = kb * chunk + lax.broadcasted_iota(jnp.int32, (chunk, rows), 0)
                qpos = qb * rows + lax.broadcasted_iota(jnp.int32, (chunk, rows), 1)
                s = jnp.where(kpos <= qpos, s, NEG_BIG)
            m_new = jnp.maximum(m, jnp.max(s, axis=0, keepdims=True))
            alpha = jnp.exp2(m - m_new)
            p = jnp.exp2(s - m_new)
            l = l * alpha + jnp.sum(p, axis=0, keepdims=True)
            vt = v_s[h * vd : (h + 1) * vd, ktok]
            acc = acc * alpha + jnp.dot(vt, p.astype(jnp.bfloat16), preferred_element_type=jnp.float32)
            new.append((m_new, l, acc))
        return tuple(new)

    carry = tuple(
        (
            jnp.full((1, rows), NEG_BIG, jnp.float32),
            jnp.zeros((1, rows), jnp.float32),
            jnp.zeros((vd, rows), jnp.float32),
        )
        for _ in range(heads)
    )
    last = (qb * rows) // chunk
    carry = lax.fori_loop(0, last, lambda kb, c: step(kb, c, False), carry)
    carry = step(last, carry, True)
    return jnp.concatenate([jnp.transpose(acc / l) for _, l, acc in carry], axis=1).astype(jnp.bfloat16)


MESH = pl.DeviceIdType.MESH


class Links:
    def __init__(self, send_sems, recv_sems):
        self.send_sems, self.recv_sems, self.ids, self.sent = send_sems, recv_sems, {}, []

    def copy(self, role, src, dst, target):
        n = self.ids.setdefault(role, len(self.ids))
        return pltpu.make_async_remote_copy(
            src_ref=src, dst_ref=dst, send_sem=self.send_sems.at[n], recv_sem=self.recv_sems.at[n],
            device_id=target, device_id_type=MESH,
        )

    def send(self, role, src, dst, target, ok=None):
        self.sent.append((ok, role, src, dst, target))
        guard(ok, lambda: self.copy(role, src, dst, target).start())

    def arrive(self, role, dst, target, ok=None):
        guard(ok, lambda: self.copy(role, dst, dst, target).wait_recv())

    def drain(self):
        for ok, role, src, dst, target in self.sent:
            guard(ok, lambda: self.copy(role, src, dst, target).wait_send())
        self.sent = []


def guard(ok, action):
    if ok is None:
        action()
    else:
        pl.when(ok)(action)


def sem_count(nx, ny, nz, cores):
    gather = 4 * ((nx - 1) * cores + cores - 1) + 2 * (nx - 1) * (ny - 1) * cores
    latent = 2 * (2 * (nz - 1) + (2 * nz - 1) * (ny - 1))
    return gather + latent


def layer_kernel(
    dims, chunk, heads, nope, vd, scale,
    tokens, in_gain, wqd, wld, wrope, q_lat_gain, kv_lat_gain, wqu, wkvu, gq, gk, tq, tk, out_gain,
    out,
    normed, wqd_g, wld_g, wqu_g, wkvu_g, wvt, kvr_g, q_g, q_s, k_s, v_s, att_s, heads_g,
    send_sems, recv_sems, a2a_send, a2a_recv,
):
    nx, ny, nz, cores = dims
    seqs, dps = ny * nz, nx * cores
    rows = tokens.shape[0]
    kr = wld.shape[1]
    s, d = lax.axis_index("sp"), lax.axis_index("dp")
    y, z = lax.rem(s, ny), lax.div(s, ny)
    c, x = lax.rem(d, cores), lax.div(d, cores)
    links = Links(send_sems, recv_sems)

    def at_sp(target):
        return {"sp": target, "dp": d}

    def at_dp(target):
        return {"sp": s, "dp": target}

    barrier = pltpu.get_barrier_semaphore()
    for k in range(1, seqs):
        pl.semaphore_signal(barrier, inc=1, device_id=at_sp(lax.rem(s + k, seqs)), device_id_type=MESH)
    for k in range(1, dps):
        pl.semaphore_signal(barrier, inc=1, device_id=at_dp(lax.rem(d + k, dps)), device_id_type=MESH)
    pl.semaphore_wait(barrier, seqs + dps - 2)

    weights = ((wqd, wqd_g, True), (wld, wld_g, True), (wqu, wqu_g, False), (wkvu, wkvu_g, False))

    def piece(ref, split, which):
        part = ref.shape[0] // ny
        return ref.at[pl.ds(pl.multiple_of(which * part, part), part)] if split else ref

    partners = [(dc, x * cores + lax.rem(c + dc, cores)) for dc in range(1, cores)]
    for a, (src, dst, split) in enumerate(weights):
        for dx in range(1, nx):
            target = lax.rem(x + dx, nx) * cores + c
            links.send(("x", a, dx), piece(src, split, y), piece(dst.at[d], split, y), at_dp(target))
        for dc, partner in partners:
            links.send(("c", a, dc), src, dst.at[d], at_dp(partner))
    for src, dst, _ in weights:
        dst[d] = src[...]

    def norm(i, _):
        step = rows // 4
        band = pl.ds(pl.multiple_of(i * step, step), step)
        normed[band, :] = rms_scale(tokens[band, :].astype(jnp.float32), in_gain[...]).astype(jnp.bfloat16)
        return 0

    lax.fori_loop(0, 4, norm, 0)

    for a, (src, dst, split) in enumerate(weights):
        for dx in range(1, nx):
            origin = lax.rem(x - dx + nx, nx) * cores + c
            got = piece(dst.at[origin], split, y)
            links.arrive(("x", a, dx), got, at_dp(d))
            for dy in range(1, ny if split else 1):
                links.send(("y", a, dx, dy), got, got, at_sp(z * ny + lax.rem(y + dy, ny)))
            for dc, partner in partners:
                links.send(("cx", a, dx, dc), got, got, at_dp(partner))
    rope_key = jnp.dot(normed[...], wrope[...], preferred_element_type=jnp.float32)
    kvr_g[s, :, kr:] = rope_key.astype(jnp.bfloat16)
    for a, (src, dst, split) in enumerate(weights):
        for dx in range(1, nx):
            origin = lax.rem(x - dx + nx, nx) * cores + c
            for dy in range(1, ny if split else 1):
                got = piece(dst.at[origin], split, lax.rem(y - dy + ny, ny))
                links.arrive(("y", a, dx, dy), got, at_dp(d))
                for dc, partner in partners:
                    links.send(("cy", a, dx, dy, dc), got, got, at_dp(partner))

    def settle(a):
        src, dst, split = weights[a]
        for dc, _ in partners:
            other = lax.rem(c - dc + cores, cores)
            links.arrive(("c", a, dc), dst.at[x * cores + other], at_dp(d))
            for dx in range(1, nx):
                origin = dst.at[lax.rem(x - dx + nx, nx) * cores + other]
                links.arrive(("cx", a, dx, dc), piece(origin, split, y), at_dp(d))
                for dy in range(1, ny if split else 1):
                    got = piece(origin, split, lax.rem(y - dy + ny, ny))
                    links.arrive(("cy", a, dx, dy, dc), got, at_dp(d))

    def down(gathered):
        part = gathered.shape[1]
        total = None
        for k in range(dps):
            term = jnp.dot(
                normed[:, k * part : (k + 1) * part], gathered[k], preferred_element_type=jnp.float32
            )
            total = term if total is None else total + term
        return total

    buffers = (kvr_g, q_g)

    def over_y(b, tag, slot, ok=None):
        block = buffers[b].at[slot]
        for dy in range(1, ny):
            links.send(("ly", b, tag, dy), block, block, at_sp(z * ny + lax.rem(y + dy, ny)), ok)

    def along_z(b, way, step, slot, ok):
        block = buffers[b].at[slot]
        links.send(("z", b, way, step), block, block, at_sp(jnp.clip(z + way, 0, nz - 1) * ny + y), ok)

    def launch(b):
        over_y(b, 0, s)
        for way in (1, -1):
            if nz > 1:
                along_z(b, way, 0, s, (z + way >= 0) & (z + way < nz))

    settle(1)
    kvr_g[s, :, :kr] = rms_scale(down(wld_g), kv_lat_gain[...]).astype(jnp.bfloat16)
    launch(0)
    settle(0)
    q_g[s] = rms_scale(down(wqd_g), q_lat_gain[...]).astype(jnp.bfloat16)
    launch(1)

    for step in range(nz - 1):
        for b in range(2):
            for way in (1, -1):
                origin = z - way * (step + 1)
                ok = (origin >= 0) & (origin < nz)
                slot = jnp.clip(origin, 0, nz - 1) * ny + y
                links.arrive(("z", b, way, step), buffers[b].at[slot], at_sp(s), ok)
                if step < nz - 2:
                    along_z(b, way, step + 1, slot, ok & (z + way >= 0) & (z + way < nz))
                over_y(b, way * (step + 1), slot, ok)
    settle(2)
    settle(3)
    wk_cols = heads * nope
    wq_full = wqu_g.reshape(dps * wqu.shape[0], wqu.shape[1])
    wkv_full = wkvu_g.reshape(dps * wkvu.shape[0], wkvu.shape[1])
    wvt[...] = jnp.transpose(wkv_full[:, wk_cols:].astype(jnp.float32)).astype(jnp.bfloat16)
    for b in range(2):
        for tag in range(1 - nz, nz):
            zz = z - tag
            ok = None if tag == 0 else (zz >= 0) & (zz < nz)
            for dy in range(1, ny):
                slot = jnp.clip(zz, 0, nz - 1) * ny + lax.rem(y - dy + ny, ny)
                links.arrive(("ly", b, tag, dy), buffers[b].at[slot], at_sp(s), ok)

    def project(i, _):
        project_block(
            i, rows, heads, nope, vd, q_g[i], kvr_g[i, :, :kr], kvr_g[i, :, kr:],
            wq_full, wkv_full.at[:, :wk_cols], wvt, gq, gk, tq, tk, q_s, k_s, v_s,
        )
        return 0

    lax.fori_loop(0, seqs, project, 0)

    def hand_over(qb):
        return pltpu.make_async_remote_copy(
            src_ref=att_s.at[qb], dst_ref=heads_g.at[s], send_sem=a2a_send.at[qb],
            recv_sem=a2a_recv.at[s], device_id=at_sp(qb), device_id_type=MESH,
        )

    def attend(i, _):
        qb = lax.rem(s + 1 + i, seqs)
        att_s[qb] = attend_block(qb, rows, chunk, heads, vd, scale, q_s, k_s, v_s)

        @pl.when(i < seqs - 1)
        def _():
            hand_over(qb).start()

        return 0

    lax.fori_loop(0, seqs, attend, 0)
    heads_g[s] = att_s[s]
    for k in range(1, seqs):
        origin = lax.rem(s + k, seqs)
        pltpu.make_async_remote_copy(
            src_ref=att_s.at[origin], dst_ref=heads_g.at[origin], send_sem=a2a_send.at[origin],
            recv_sem=a2a_recv.at[origin], device_id=at_sp(origin), device_id_type=MESH,
        ).wait()
    links.drain()

    width = heads * vd
    square = jnp.zeros((rows, 1), jnp.float32)
    for k in range(seqs):
        block = heads_g[k].astype(jnp.float32)
        square = square + jnp.sum(block * block, axis=-1, keepdims=True)
    r = lax.rsqrt(square * (1.0 / (seqs * width)) + EPS)
    for k in range(seqs):
        cols = slice(k * width, (k + 1) * width)
        out[:, cols] = (heads_g[k].astype(jnp.float32) * r * out_gain[:, cols]).astype(jnp.bfloat16)


def per_device(
    tokens, in_gain, w_query_down, w_latent_down, w_rope_key, query_latent_gain, latent_gain,
    w_query_up, w_key_up, w_value_up, query_gain, key_gain, out_gain, w_out,
):
    seqs, dps = lax.axis_size("sp"), lax.axis_size("dp")
    cores = 2 if dps % 2 == 0 else 1
    nx = dps // cores
    ny = nx if seqs % nx == 0 else 1
    nz = seqs // ny
    heads = HEADS // seqs
    own_rows = tokens.shape[1]
    length = own_rows * seqs
    rope = w_rope_key.shape[1]
    nope = w_key_up.shape[1] // heads
    vd = w_value_up.shape[1] // heads
    wide = nope + 2 * rope
    out_full = lax.all_gather(w_out, ("sp", "dp"), axis=0, tiled=True)
    tq, tk = tables(length, rope, (query_gain, key_gain))
    wide_rope = jnp.concatenate([w_rope_key, swap_halves(w_rope_key)], axis=1)
    wqu = widen_query(w_query_up, heads, rope)
    wkvu = jnp.concatenate([w_key_up, w_value_up], axis=1)
    chunk = min(2 * own_rows, length)
    sems = sem_count(nx, ny, nz, cores)
    b16 = jnp.bfloat16

    def gathered(w):
        return pltpu.VMEM((dps,) + w.shape, b16)

    mixed = pl.pallas_call(
        functools.partial(
            layer_kernel, (nx, ny, nz, cores), chunk, heads, nope, vd, float(nope + rope) ** -0.5
        ),
        out_shape=jax.ShapeDtypeStruct((own_rows, seqs * heads * vd), b16),
        in_specs=[pl.BlockSpec(memory_space=pltpu.VMEM)] * 14,
        out_specs=pl.BlockSpec(memory_space=pltpu.VMEM),
        scratch_shapes=[
            pltpu.VMEM((own_rows, tokens.shape[2]), b16),
            gathered(w_query_down), gathered(w_latent_down), gathered(wqu), gathered(wkvu),
            pltpu.VMEM((heads * vd, w_latent_down.shape[1]), b16),
            pltpu.VMEM((seqs, own_rows, w_latent_down.shape[1] + 2 * rope), b16),
            pltpu.VMEM((seqs, own_rows, w_query_down.shape[1]), b16),
            pltpu.VMEM((heads, length, wide), b16),
            pltpu.VMEM((heads, length, wide), b16),
            pltpu.VMEM((heads * vd, length), b16),
            pltpu.VMEM((seqs, own_rows, heads * vd), b16),
            pltpu.VMEM((seqs, own_rows, heads * vd), b16),
            pltpu.SemaphoreType.DMA((sems,)),
            pltpu.SemaphoreType.DMA((sems,)),
            pltpu.SemaphoreType.DMA((seqs,)),
            pltpu.SemaphoreType.DMA((seqs,)),
        ],
        compiler_params=pltpu.CompilerParams(
            vmem_limit_bytes=56 * 1024 * 1024, collective_id=0, has_side_effects=True
        ),
        cost_estimate=pl.CostEstimate(flops=60 * 10**9, bytes_accessed=10**8, transcendentals=5 * 10**6),
    )(
        tokens.reshape(own_rows, tokens.shape[2]), in_gain[None], w_query_down, w_latent_down, wide_rope,
        query_latent_gain[None], latent_gain[None], wqu, wkvu,
        query_gain[None, :nope], key_gain[None, :nope], tq, tk, out_gain[None],
    )
    projected = jnp.dot(mixed, out_full, preferred_element_type=jnp.float32)
    return projected.astype(b16).reshape(1, own_rows, w_out.shape[1])


def solution(mesh):
    in_specs = (
        P("dp", "sp", None), P(), P("dp", None), P("dp", None), P(), P(), P(),
        P("dp", "sp"), P("dp", "sp"), P("dp", "sp"), P(), P(), P(), P(("sp", "dp"), None),
    )
    return jax.shard_map(
        per_device, mesh=mesh, in_specs=in_specs, out_specs=P("dp", "sp", None), check_vma=False
    )
```

```python
import functools

import jax
import jax.numpy as jnp
import numpy as np
from jax import lax
from jax.experimental import pallas as pl
from jax.experimental.pallas import tpu as pltpu
from jax.sharding import PartitionSpec as P

HEADS = 16
EPS = 1e-06
THETA = 10000.0
NEG_BIG = -1e30
LOG2E = 1.4426950408889634
NT = (((1,), (1,)), ((), ()))


def rms_scale(values, scaling):
    return values * lax.rsqrt(jnp.mean(values * values, axis=-1, keepdims=True) + EPS) * scaling


def swap_halves(x):
    half = x.shape[-1] // 2
    return jnp.concatenate([x[..., half:], x[..., :half]], axis=-1)


def rotation_table(length, width):
    half = width // 2
    frequency = np.float32(THETA) ** (-np.arange(half, dtype=np.float32) / np.float32(half))
    angles = np.arange(length, dtype=np.float32)[:, None] * frequency[None, :]
    cosine, sine = np.cos(angles), np.sin(angles)
    return np.concatenate([cosine, cosine, -sine, sine], axis=-1).astype(np.float32)


def with_swapped(x):
    return jnp.concatenate([x, swap_halves(x)], axis=-1)


def project_block(i, rows, heads, nope, vd, lq, lkv, rp, wq, wk, wvt, gq, gk, gq2, gk2, table, q_s, k_s, v_s):
    tok = pl.ds(pl.multiple_of(i * rows, rows), rows)
    wide = wq.shape[1] // heads
    rope2 = wide - nope
    inv = 1.0 / (nope + rope2 // 2)
    q = jnp.dot(lq, wq[...], preferred_element_type=jnp.float32)
    k = jnp.dot(lkv, wk[...], preferred_element_type=jnp.float32)
    v_s[:, tok] = lax.dot_general(wvt[...], lkv, NT, preferred_element_type=jnp.float32).astype(jnp.bfloat16)
    shared = rp.astype(jnp.float32)
    shared_sq = 0.5 * shared * shared
    lane = lax.broadcasted_iota(jnp.int32, (rows, rope2), 1)
    tqv, tkv = table[tok, :] * gq2, table[tok, :] * gk2
    for h in range(heads):
        for which in range(2):
            if which == 0:
                t1 = q[:, h * wide : h * wide + nope]
                t2 = q[:, h * wide + nope : (h + 1) * wide]
                sq, gain, turn, dest = t1 * t1 + 0.5 * t2 * t2, gq, tqv, q_s
            else:
                t1, t2 = k[:, h * nope : (h + 1) * nope], shared
                sq, gain, turn, dest = t1 * t1 + shared_sq, gk, tkv, k_s
            r = lax.rsqrt(jnp.sum(sq, axis=-1, keepdims=True) * inv + EPS)
            dest[h, tok, 0:nope] = (t1 * r * gain).astype(jnp.bfloat16)
            y = t2 * r * turn
            y = y + pltpu.roll(y, rope2 // 2, 1)
            if which == 1:
                y = jnp.where(lane < rope2 // 2, y, 0.0)
            dest[h, tok, nope:wide] = y.astype(jnp.bfloat16)


def attend_block(qb, rows, chunk, heads, vd, scale, q_s, k_s, v_s):
    qtok = pl.ds(pl.multiple_of(qb * rows, rows), rows)
    qs = [q_s[h, qtok, :] for h in range(heads)]
    factor = scale * LOG2E

    def step(kb, carry, masked):
        ktok = pl.ds(pl.multiple_of(kb * chunk, chunk), chunk)
        new = []
        for h in range(heads):
            m, l, acc = carry[h]
            s = lax.dot_general(k_s[h, ktok, :], qs[h], NT, preferred_element_type=jnp.float32) * factor
            if masked:
                kpos = kb * chunk + lax.broadcasted_iota(jnp.int32, (chunk, rows), 0)
                qpos = qb * rows + lax.broadcasted_iota(jnp.int32, (chunk, rows), 1)
                s = jnp.where(kpos <= qpos, s, NEG_BIG)
            m_new = jnp.maximum(m, jnp.max(s, axis=0, keepdims=True))
            alpha = jnp.exp2(m - m_new)
            p = jnp.exp2(s - m_new)
            l = l * alpha + jnp.sum(p, axis=0, keepdims=True)
            vt = v_s[h * vd : (h + 1) * vd, ktok]
            acc = acc * alpha + jnp.dot(vt, p.astype(jnp.bfloat16), preferred_element_type=jnp.float32)
            new.append((m_new, l, acc))
        return tuple(new)

    carry = tuple(
        (
            jnp.full((1, rows), NEG_BIG, jnp.float32),
            jnp.zeros((1, rows), jnp.float32),
            jnp.zeros((vd, rows), jnp.float32),
        )
        for _ in range(heads)
    )
    last = (qb * rows) // chunk
    carry = lax.fori_loop(0, last, lambda kb, c: step(kb, c, False), carry)
    carry = step(last, carry, True)
    return jnp.concatenate([jnp.transpose(acc / l) for _, l, acc in carry], axis=1).astype(jnp.bfloat16)


MESH = pl.DeviceIdType.MESH


class Links:
    def __init__(self, send_sems, recv_sems):
        self.send_sems, self.recv_sems, self.ids, self.sent = send_sems, recv_sems, {}, []

    def copy(self, role, src, dst, target):
        n = self.ids.setdefault(role, len(self.ids))
        return pltpu.make_async_remote_copy(
            src_ref=src, dst_ref=dst, send_sem=self.send_sems.at[n], recv_sem=self.recv_sems.at[n],
            device_id=target, device_id_type=MESH,
        )

    def send(self, role, src, dst, target, ok=None):
        self.sent.append((ok, role, src, dst, target))
        guard(ok, lambda: self.copy(role, src, dst, target).start())

    def arrive(self, role, dst, target, ok=None):
        guard(ok, lambda: self.copy(role, dst, dst, target).wait_recv())

    def drain(self):
        for ok, role, src, dst, target in self.sent:
            guard(ok, lambda: self.copy(role, src, dst, target).wait_send())
        self.sent = []


def guard(ok, action):
    if ok is None:
        action()
    else:
        pl.when(ok)(action)


def sem_count(nx, ny, nz, cores):
    gather = 5 * ((nx - 1) * cores + cores - 1) + 2 * (nx - 1) * (ny - 1) * cores
    latent = 2 * (2 * (nz - 1) + (2 * nz - 1) * (ny - 1))
    out = 2 * (nz - 1) + nz * (ny - 1) + nz * ny * (nx - 1) + nz * ny * nx * (cores - 1)
    return gather + latent + out


def layer_kernel(
    dims, chunk, heads, nope, vd, scale,
    tokens, in_gain, wqd, wld, wrope, q_lat_gain, kv_lat_gain, wqu, wku, wvu, q_gain, k_gain, table, out_gain, w_out,
    out,
    normed, wqd_g, wld_g, wqu_g, wku_g, wvu_g, w_g, wq_s, wvt, kvr_g, q_g, q_s, k_s, v_s, att_s, heads_g,
    send_sems, recv_sems, a2a_send, a2a_recv,
):
    nx, ny, nz, cores = dims
    seqs, dps = ny * nz, nx * cores
    rows = tokens.shape[0]
    kr = wld.shape[1]
    s, d = lax.axis_index("sp"), lax.axis_index("dp")
    y, z = lax.rem(s, ny), lax.div(s, ny)
    c, x = lax.rem(d, cores), lax.div(d, cores)
    links = Links(send_sems, recv_sems)

    def at_sp(target):
        return {"sp": target, "dp": d}

    def at_dp(target):
        return {"sp": s, "dp": target}

    barrier = pltpu.get_barrier_semaphore()
    for k in range(1, seqs):
        pl.semaphore_signal(barrier, inc=1, device_id=at_sp(lax.rem(s + k, seqs)), device_id_type=MESH)
    for k in range(1, dps):
        pl.semaphore_signal(barrier, inc=1, device_id=at_dp(lax.rem(d + k, dps)), device_id_type=MESH)
    pl.semaphore_wait(barrier, seqs + dps - 2)

    weights = ((wqd, wqd_g, True), (wld, wld_g, True), (wqu, wqu_g, False), (wku, wku_g, False), (wvu, wvu_g, False))

    def piece(ref, split, which):
        part = ref.shape[0] // ny
        return ref.at[pl.ds(pl.multiple_of(which * part, part), part)] if split else ref

    partners = [(dc, x * cores + lax.rem(c + dc, cores)) for dc in range(1, cores)]
    for a, (src, dst, split) in enumerate(weights):
        for dx in range(1, nx):
            target = lax.rem(x + dx, nx) * cores + c
            links.send(("x", a, dx), piece(src, split, y), piece(dst.at[d], split, y), at_dp(target))
        for dc, partner in partners:
            links.send(("c", a, dc), src, dst.at[d], at_dp(partner))

    part_out = w_out.shape[0]

    def w_block(zz, yy, xx, cc):
        first = ((zz * ny + yy) * dps + xx * cores + cc) * part_out
        return w_g.at[pl.ds(pl.multiple_of(first, part_out), part_out)]

    def w_z(way, step, src, dst, ok):
        links.send(("wz", way, step), src, dst, at_sp(jnp.clip(z + way, 0, nz - 1) * ny + y), ok)

    def w_z_step(step):
        for way in (1, -1):
            origin = z - way * (step + 1)
            ok = (origin >= 0) & (origin < nz)
            block = w_block(jnp.clip(origin, 0, nz - 1), y, x, c)
            links.arrive(("wz", way, step), block, at_sp(s), ok)
            if step < nz - 2:
                w_z(way, step + 1, block, block, ok & (z + way >= 0) & (z + way < nz))

    def w_x(k, dy):
        block = w_block(lax.rem(z + k, nz), lax.rem(y - dy + ny, ny), x, c)
        for dx in range(1, nx):
            links.send(("wx", k, dy, dx), block, block, at_dp(lax.rem(x + dx, nx) * cores + c))
        w_core(k, dy, 0, block)

    def w_core(k, dy, dx, block):
        for dc, partner in partners:
            links.send(("wc", k, dy, dx, dc), block, block, at_dp(partner))

    def w_x_arrive(k, dy):
        for dx in range(1, nx):
            block = w_block(lax.rem(z + k, nz), lax.rem(y - dy + ny, ny), lax.rem(x - dx + nx, nx), c)
            links.arrive(("wx", k, dy, dx), block, at_dp(d))
            w_core(k, dy, dx, block)

    for way in (1, -1):
        if nz > 1:
            w_z(way, 0, w_out, w_block(z, y, x, c), (z + way >= 0) & (z + way < nz))
    for src, dst, _ in weights:
        dst[d] = src[...]
    own_out = pl.ds(pl.multiple_of((s * dps + d) * part_out, part_out), part_out)
    w_g[own_out, :] = w_out[...]

    def norm(i, _):
        step = rows // 4
        band = pl.ds(pl.multiple_of(i * step, step), step)
        normed[band, :] = rms_scale(tokens[band, :].astype(jnp.float32), in_gain[...]).astype(jnp.bfloat16)
        return 0

    lax.fori_loop(0, 4, norm, 0)

    for a, (src, dst, split) in enumerate(weights):
        for dx in range(1, nx):
            origin = lax.rem(x - dx + nx, nx) * cores + c
            got = piece(dst.at[origin], split, y)
            links.arrive(("x", a, dx), got, at_dp(d))
            for dy in range(1, ny if split else 1):
                links.send(("y", a, dx, dy), got, got, at_sp(z * ny + lax.rem(y + dy, ny)))
            for dc, partner in partners:
                links.send(("cx", a, dx, dc), got, got, at_dp(partner))
    rope_key = jnp.dot(normed[...], wrope[...], preferred_element_type=jnp.float32)
    kvr_g[s, :, kr:] = with_swapped(rope_key).astype(jnp.bfloat16)
    for a, (src, dst, split) in enumerate(weights):
        for dx in range(1, nx):
            origin = lax.rem(x - dx + nx, nx) * cores + c
            for dy in range(1, ny if split else 1):
                got = piece(dst.at[origin], split, lax.rem(y - dy + ny, ny))
                links.arrive(("y", a, dx, dy), got, at_dp(d))
                for dc, partner in partners:
                    links.send(("cy", a, dx, dy, dc), got, got, at_dp(partner))

    def settle(a):
        src, dst, split = weights[a]
        for dc, _ in partners:
            other = lax.rem(c - dc + cores, cores)
            links.arrive(("c", a, dc), dst.at[x * cores + other], at_dp(d))
            for dx in range(1, nx):
                origin = dst.at[lax.rem(x - dx + nx, nx) * cores + other]
                links.arrive(("cx", a, dx, dc), piece(origin, split, y), at_dp(d))
                for dy in range(1, ny if split else 1):
                    got = piece(origin, split, lax.rem(y - dy + ny, ny))
                    links.arrive(("cy", a, dx, dy, dc), got, at_dp(d))

    def down(gathered):
        part = gathered.shape[1]
        total = None
        for k in range(dps):
            term = jnp.dot(
                normed[:, k * part : (k + 1) * part], gathered[k], preferred_element_type=jnp.float32
            )
            total = term if total is None else total + term
        return total

    buffers = (kvr_g, q_g)

    def over_y(b, tag, slot, ok=None):
        block = buffers[b].at[slot]
        for dy in range(1, ny):
            links.send(("ly", b, tag, dy), block, block, at_sp(z * ny + lax.rem(y + dy, ny)), ok)

    def along_z(b, way, step, slot, ok):
        block = buffers[b].at[slot]
        links.send(("z", b, way, step), block, block, at_sp(jnp.clip(z + way, 0, nz - 1) * ny + y), ok)

    def launch(b):
        over_y(b, 0, s)
        for way in (1, -1):
            if nz > 1:
                along_z(b, way, 0, s, (z + way >= 0) & (z + way < nz))

    if nz > 1:
        w_z_step(0)
    settle(1)
    kvr_g[s, :, :kr] = rms_scale(down(wld_g), kv_lat_gain[...]).astype(jnp.bfloat16)
    launch(0)
    settle(0)
    q_g[s] = rms_scale(down(wqd_g), q_lat_gain[...]).astype(jnp.bfloat16)
    launch(1)
    for step in range(1, nz - 1):
        w_z_step(step)
    for k in range(nz):
        w_x(k, 0)

    for step in range(nz - 1):
        for b in range(2):
            for way in (1, -1):
                origin = z - way * (step + 1)
                ok = (origin >= 0) & (origin < nz)
                slot = jnp.clip(origin, 0, nz - 1) * ny + y
                links.arrive(("z", b, way, step), buffers[b].at[slot], at_sp(s), ok)
                if step < nz - 2:
                    along_z(b, way, step + 1, slot, ok & (z + way >= 0) & (z + way < nz))
                over_y(b, way * (step + 1), slot, ok)
    for k in range(nz):
        for dy in range(1, ny):
            block = w_block(lax.rem(z + k, nz), y, x, c)
            links.send(("wy", k, dy), block, block, at_sp(z * ny + lax.rem(y + dy, ny)))
    settle(2)
    settle(3)
    settle(4)
    wk_full = wku_g.reshape(dps * wku.shape[0], wku.shape[1])
    for k in range(dps):
        depth = wqu.shape[0]
        up = wqu_g[k].astype(jnp.float32)
        columns = []
        for h in range(heads):
            head = up[:, h * (wqu.shape[1] // heads) : (h + 1) * (wqu.shape[1] // heads)]
            columns += [head[:, :nope], with_swapped(head[:, nope:])]
        wq_s[k * depth : (k + 1) * depth, :] = jnp.concatenate(columns, axis=1).astype(jnp.bfloat16)
    wv_full = wvu_g.reshape(dps * wvu.shape[0], wvu.shape[1])
    wvt[...] = jnp.transpose(wv_full[...].astype(jnp.float32)).astype(jnp.bfloat16)
    gq, gk = q_gain[:, :nope], k_gain[:, :nope]
    gq2, gk2 = with_swapped(q_gain[:, nope:]), with_swapped(k_gain[:, nope:])
    for b in range(2):
        for tag in range(1 - nz, nz):
            zz = z - tag
            ok = None if tag == 0 else (zz >= 0) & (zz < nz)
            for dy in range(1, ny):
                slot = jnp.clip(zz, 0, nz - 1) * ny + lax.rem(y - dy + ny, ny)
                links.arrive(("ly", b, tag, dy), buffers[b].at[slot], at_sp(s), ok)

    def project(i, _):
        project_block(
            i, rows, heads, nope, vd, q_g[i], kvr_g[i, :, :kr], kvr_g[i, :, kr:],
            wq_s, wk_full, wvt, gq, gk, gq2, gk2, table, q_s, k_s, v_s,
        )
        return 0

    lax.fori_loop(0, seqs, project, 0)

    def hand_over(qb):
        return pltpu.make_async_remote_copy(
            src_ref=att_s.at[qb], dst_ref=heads_g.at[s], send_sem=a2a_send.at[qb],
            recv_sem=a2a_recv.at[s], device_id=at_sp(qb), device_id_type=MESH,
        )

    def attend(i, _):
        qb = lax.rem(s + 1 + i, seqs)
        att_s[qb] = attend_block(qb, rows, chunk, heads, vd, scale, q_s, k_s, v_s)

        @pl.when(i < seqs - 1)
        def _():
            hand_over(qb).start()

        return 0

    lax.fori_loop(0, seqs // 2, attend, 0)
    for k in range(nz):
        for dy in range(1, ny):
            block = w_block(lax.rem(z + k, nz), lax.rem(y - dy + ny, ny), x, c)
            links.arrive(("wy", k, dy), block, at_sp(s))
            w_x(k, dy)
    for k in range(nz):
        w_x_arrive(k, 0)
    lax.fori_loop(seqs // 2, seqs, attend, 0)
    for k in range(nz):
        for dy in range(1, ny):
            w_x_arrive(k, dy)
    heads_g[s] = att_s[s]
    for k in range(1, seqs):
        origin = lax.rem(s + k, seqs)
        pltpu.make_async_remote_copy(
            src_ref=att_s.at[origin], dst_ref=heads_g.at[origin], send_sem=a2a_send.at[origin],
            recv_sem=a2a_recv.at[origin], device_id=at_sp(origin), device_id_type=MESH,
        ).wait()
    width = heads * vd
    square = jnp.zeros((rows, 1), jnp.float32)
    for k in range(seqs):
        block = heads_g[k].astype(jnp.float32)
        square = square + jnp.sum(block * block, axis=-1, keepdims=True)
    r = lax.rsqrt(square * (1.0 / (seqs * width)) + EPS)
    for k in range(seqs):
        cols = slice(k * width, (k + 1) * width)
        normed[:, cols] = (heads_g[k].astype(jnp.float32) * r * out_gain[:, cols]).astype(jnp.bfloat16)
    for k in range(nz):
        for dy in range(ny):
            for dx in range(nx):
                for dc, _ in partners:
                    block = w_block(
                        lax.rem(z + k, nz), lax.rem(y - dy + ny, ny), lax.rem(x - dx + nx, nx),
                        lax.rem(c - dc + cores, cores),
                    )
                    links.arrive(("wc", k, dy, dx, dc), block, at_dp(d))
    tile = 256 if out.shape[1] % 256 == 0 else out.shape[1]

    def project_out(i, _):
        cols = pl.ds(pl.multiple_of(i * tile, tile), tile)
        out[:, cols] = jnp.dot(normed[...], w_g[:, cols], preferred_element_type=jnp.float32).astype(out.dtype)
        return 0

    lax.fori_loop(0, out.shape[1] // tile, project_out, 0)
    links.drain()


def per_device(
    tokens, in_gain, w_query_down, w_latent_down, w_rope_key, query_latent_gain, latent_gain,
    w_query_up, w_key_up, w_value_up, query_gain, key_gain, out_gain, w_out,
):
    seqs, dps = lax.axis_size("sp"), lax.axis_size("dp")
    cores = 2 if dps % 2 == 0 else 1
    nx = dps // cores
    ny = nx if seqs % nx == 0 else 1
    nz = seqs // ny
    heads = HEADS // seqs
    own_rows = tokens.shape[1]
    length = own_rows * seqs
    rope = w_rope_key.shape[1]
    nope = w_key_up.shape[1] // heads
    vd = w_value_up.shape[1] // heads
    wide = nope + 2 * rope
    chunk = min(2 * own_rows, length)
    sems = sem_count(nx, ny, nz, cores)
    b16 = jnp.bfloat16

    def gathered(w):
        return pltpu.VMEM((dps,) + w.shape, b16)

    result = pl.pallas_call(
        functools.partial(
            layer_kernel, (nx, ny, nz, cores), chunk, heads, nope, vd, float(nope + rope) ** -0.5
        ),
        out_shape=jax.ShapeDtypeStruct((own_rows, w_out.shape[1]), b16),
        in_specs=[pl.BlockSpec(memory_space=pltpu.VMEM)] * 15,
        out_specs=pl.BlockSpec(memory_space=pltpu.VMEM),
        scratch_shapes=[
            pltpu.VMEM((own_rows, max(tokens.shape[2], w_out.shape[0] * seqs * dps)), b16),
            gathered(w_query_down), gathered(w_latent_down), gathered(w_query_up), gathered(w_key_up), gathered(w_value_up),
            pltpu.VMEM((w_out.shape[0] * seqs * dps, w_out.shape[1]), b16),
            pltpu.VMEM((w_query_down.shape[1], heads * wide), b16),
            pltpu.VMEM((heads * vd, w_latent_down.shape[1]), b16),
            pltpu.VMEM((seqs, own_rows, w_latent_down.shape[1] + 2 * rope), b16),
            pltpu.VMEM((seqs, own_rows, w_query_down.shape[1]), b16),
            pltpu.VMEM((heads, length, wide), b16),
            pltpu.VMEM((heads, length, wide), b16),
            pltpu.VMEM((heads * vd, length), b16),
            pltpu.VMEM((seqs, own_rows, heads * vd), b16),
            pltpu.VMEM((seqs, own_rows, heads * vd), b16),
            pltpu.SemaphoreType.DMA((sems,)),
            pltpu.SemaphoreType.DMA((sems,)),
            pltpu.SemaphoreType.DMA((seqs,)),
            pltpu.SemaphoreType.DMA((seqs,)),
        ],
        compiler_params=pltpu.CompilerParams(
            vmem_limit_bytes=56 * 1024 * 1024, collective_id=0, has_side_effects=True
        ),
        cost_estimate=pl.CostEstimate(flops=60 * 10**9, bytes_accessed=10**8, transcendentals=5 * 10**6),
    )(
        tokens.reshape(own_rows, tokens.shape[2]), in_gain[None], w_query_down, w_latent_down, w_rope_key,
        query_latent_gain[None], latent_gain[None], w_query_up, w_key_up, w_value_up,
        query_gain[None], key_gain[None], jnp.asarray(rotation_table(length, rope)), out_gain[None], w_out,
    )
    return result.reshape(1, own_rows, w_out.shape[1])


def solution(mesh):
    in_specs = (
        P("dp", "sp", None), P(), P("dp", None), P("dp", None), P(), P(), P(),
        P("dp", "sp"), P("dp", "sp"), P("dp", "sp"), P(), P(), P(), P(("sp", "dp"), None),
    )
    return jax.shard_map(
        per_device, mesh=mesh, in_specs=in_specs, out_specs=P("dp", "sp", None), check_vma=False
    )
```

```python
import functools

import jax
import jax.numpy as jnp
import numpy as np
from jax import lax
from jax.experimental import pallas as pl
from jax.experimental.pallas import tpu as pltpu
from jax.sharding import PartitionSpec as P

HEADS = 16
EPS = 1e-06
THETA = 10000.0
NEG_BIG = -1e30
LOG2E = 1.4426950408889634
NT = (((1,), (1,)), ((), ()))


def rms_scale(values, scaling):
    return values * lax.rsqrt(jnp.mean(values * values, axis=-1, keepdims=True) + EPS) * scaling


def swap_halves(x):
    half = x.shape[-1] // 2
    return jnp.concatenate([x[..., half:], x[..., :half]], axis=-1)


def rotation_table(length, width):
    half = width // 2
    frequency = np.float32(THETA) ** (-np.arange(half, dtype=np.float32) / np.float32(half))
    angles = np.arange(length, dtype=np.float32)[:, None] * frequency[None, :]
    cosine, sine = np.cos(angles), np.sin(angles)
    return np.concatenate([cosine, cosine, -sine, sine], axis=-1).astype(np.float32)


def with_swapped(x):
    return jnp.concatenate([x, swap_halves(x)], axis=-1)


def project_block(i, rows, heads, nope, vd, lq, lkv, rp, wq, wk, wvt, gq, gk, gq2, gk2, table, q_s, k_s, v_s):
    tok = pl.ds(pl.multiple_of(i * rows, rows), rows)
    wide = wq.shape[1] // heads
    rope2 = wide - nope
    inv = 1.0 / (nope + rope2 // 2)
    q = jnp.dot(lq, wq[...], preferred_element_type=jnp.float32)
    k = jnp.dot(lkv, wk[...], preferred_element_type=jnp.float32)
    v_s[:, tok] = lax.dot_general(wvt[...], lkv, NT, preferred_element_type=jnp.float32).astype(jnp.bfloat16)
    shared = rp.astype(jnp.float32)
    shared_sq = 0.5 * shared * shared
    lane = lax.broadcasted_iota(jnp.int32, (rows, rope2), 1)
    tqv, tkv = table[tok, :] * gq2, table[tok, :] * gk2
    for h in range(heads):
        for which in range(2):
            if which == 0:
                t1 = q[:, h * wide : h * wide + nope]
                t2 = q[:, h * wide + nope : (h + 1) * wide]
                sq, gain, turn, dest = t1 * t1 + 0.5 * t2 * t2, gq, tqv, q_s
            else:
                t1, t2 = k[:, h * nope : (h + 1) * nope], shared
                sq, gain, turn, dest = t1 * t1 + shared_sq, gk, tkv, k_s
            r = lax.rsqrt(jnp.sum(sq, axis=-1, keepdims=True) * inv + EPS)
            dest[h, tok, 0:nope] = (t1 * r * gain).astype(jnp.bfloat16)
            y = t2 * r * turn
            y = y + pltpu.roll(y, rope2 // 2, 1)
            if which == 1:
                y = jnp.where(lane < rope2 // 2, y, 0.0)
            dest[h, tok, nope:wide] = y.astype(jnp.bfloat16)


def attend_block(qb, rows, chunk, heads, vd, scale, q_s, k_s, v_s):
    qtok = pl.ds(pl.multiple_of(qb * rows, rows), rows)
    qs = [q_s[h, qtok, :] for h in range(heads)]
    factor = scale * LOG2E

    def step(kb, carry, masked):
        ktok = pl.ds(pl.multiple_of(kb * chunk, chunk), chunk)
        new = []
        for h in range(heads):
            m, l, acc = carry[h]
            s = lax.dot_general(k_s[h, ktok, :], qs[h], NT, preferred_element_type=jnp.float32) * factor
            if masked:
                kpos = kb * chunk + lax.broadcasted_iota(jnp.int32, (chunk, rows), 0)
                qpos = qb * rows + lax.broadcasted_iota(jnp.int32, (chunk, rows), 1)
                s = jnp.where(kpos <= qpos, s, NEG_BIG)
            m_new = jnp.maximum(m, jnp.max(s, axis=0, keepdims=True))
            alpha = jnp.exp2(m - m_new)
            p = jnp.exp2(s - m_new)
            l = l * alpha + jnp.sum(p, axis=0, keepdims=True)
            vt = v_s[h * vd : (h + 1) * vd, ktok]
            acc = acc * alpha + jnp.dot(vt, p.astype(jnp.bfloat16), preferred_element_type=jnp.float32)
            new.append((m_new, l, acc))
        return tuple(new)

    carry = tuple(
        (
            jnp.full((1, rows), NEG_BIG, jnp.float32),
            jnp.zeros((1, rows), jnp.float32),
            jnp.zeros((vd, rows), jnp.float32),
        )
        for _ in range(heads)
    )
    last = (qb * rows) // chunk
    carry = lax.fori_loop(0, last, lambda kb, c: step(kb, c, False), carry)
    carry = step(last, carry, True)
    return jnp.concatenate([jnp.transpose(acc / l) for _, l, acc in carry], axis=1).astype(jnp.bfloat16)


MESH = pl.DeviceIdType.MESH


class Links:
    def __init__(self, send_sems, recv_sems):
        self.send_sems, self.recv_sems, self.ids, self.sent = send_sems, recv_sems, {}, []

    def copy(self, role, src, dst, target):
        n = self.ids.setdefault(role, len(self.ids))
        return pltpu.make_async_remote_copy(
            src_ref=src, dst_ref=dst, send_sem=self.send_sems.at[n], recv_sem=self.recv_sems.at[n],
            device_id=target, device_id_type=MESH,
        )

    def send(self, role, src, dst, target, ok=None):
        self.sent.append((ok, role, src, dst, target))
        guard(ok, lambda: self.copy(role, src, dst, target).start())

    def arrive(self, role, dst, target, ok=None):
        guard(ok, lambda: self.copy(role, dst, dst, target).wait_recv())

    def drain(self):
        for ok, role, src, dst, target in self.sent:
            guard(ok, lambda: self.copy(role, src, dst, target).wait_send())
        self.sent = []


def guard(ok, action):
    if ok is None:
        action()
    else:
        pl.when(ok)(action)


def sem_count(nx, ny, nz, cores):
    gather = 5 * ((nx - 1) * cores + cores - 1) + 2 * (nx - 1) * (ny - 1) * cores
    latent = 2 * (2 * (nz - 1) + (2 * nz - 1) * (ny - 1))
    out = 2 * (nz - 1) + nz * (ny - 1) + nz * ny * (nx - 1) + nz * ny * nx * (cores - 1)
    return gather + latent + out


def layer_kernel(
    dims, chunk, heads, nope, vd, scale,
    tokens, in_gain, wqd, wld, wrope, q_lat_gain, kv_lat_gain, wqu, wku, wvu, q_gain, k_gain, table, out_gain, w_out,
    out,
    normed, wqd_g, wld_g, wqu_g, wku_g, wvu_g, w_g, wq_s, wvt, kvr_g, q_g, q_s, k_s, v_s, att_s, heads_g,
    send_sems, recv_sems, a2a_send, a2a_recv,
):
    nx, ny, nz, cores = dims
    seqs, dps = ny * nz, nx * cores
    rows = tokens.shape[0]
    kr = wld.shape[1]
    s, d = lax.axis_index("sp"), lax.axis_index("dp")
    y, z = lax.rem(s, ny), lax.div(s, ny)
    c, x = lax.rem(d, cores), lax.div(d, cores)
    links = Links(send_sems, recv_sems)

    def at_sp(target):
        return {"sp": target, "dp": d}

    def at_dp(target):
        return {"sp": s, "dp": target}

    barrier = pltpu.get_barrier_semaphore()
    for k in range(1, seqs):
        pl.semaphore_signal(barrier, inc=1, device_id=at_sp(lax.rem(s + k, seqs)), device_id_type=MESH)
    for k in range(1, dps):
        pl.semaphore_signal(barrier, inc=1, device_id=at_dp(lax.rem(d + k, dps)), device_id_type=MESH)
    pl.semaphore_wait(barrier, seqs + dps - 2)

    weights = ((wld, wld_g, True), (wqd, wqd_g, True), (wqu, wqu_g, False), (wku, wku_g, False), (wvu, wvu_g, False))

    def piece(ref, split, which):
        part = ref.shape[0] // ny
        return ref.at[pl.ds(pl.multiple_of(which * part, part), part)] if split else ref

    partners = [(dc, x * cores + lax.rem(c + dc, cores)) for dc in range(1, cores)]
    for a, (src, dst, split) in enumerate(weights):
        for dx in range(1, nx):
            target = lax.rem(x + dx, nx) * cores + c
            links.send(("x", a, dx), piece(src, split, y), piece(dst.at[d], split, y), at_dp(target))
        for dc, partner in partners:
            links.send(("c", a, dc), src, dst.at[d], at_dp(partner))

    part_out = w_out.shape[0]

    def w_block(zz, yy, xx, cc):
        first = ((zz * ny + yy) * dps + xx * cores + cc) * part_out
        return w_g.at[pl.ds(pl.multiple_of(first, part_out), part_out)]

    def w_z(way, step, src, dst, ok):
        links.send(("wz", way, step), src, dst, at_sp(jnp.clip(z + way, 0, nz - 1) * ny + y), ok)

    def w_z_step(step):
        for way in (1, -1):
            origin = z - way * (step + 1)
            ok = (origin >= 0) & (origin < nz)
            block = w_block(jnp.clip(origin, 0, nz - 1), y, x, c)
            links.arrive(("wz", way, step), block, at_sp(s), ok)
            if step < nz - 2:
                w_z(way, step + 1, block, block, ok & (z + way >= 0) & (z + way < nz))

    def w_x(k, dy):
        block = w_block(lax.rem(z + k, nz), lax.rem(y - dy + ny, ny), x, c)
        for dx in range(1, nx):
            links.send(("wx", k, dy, dx), block, block, at_dp(lax.rem(x + dx, nx) * cores + c))
        w_core(k, dy, 0, block)

    def w_core(k, dy, dx, block):
        for dc, partner in partners:
            links.send(("wc", k, dy, dx, dc), block, block, at_dp(partner))

    def w_x_arrive(k, dy):
        for dx in range(1, nx):
            block = w_block(lax.rem(z + k, nz), lax.rem(y - dy + ny, ny), lax.rem(x - dx + nx, nx), c)
            links.arrive(("wx", k, dy, dx), block, at_dp(d))
            w_core(k, dy, dx, block)

    for way in (1, -1):
        if nz > 1:
            w_z(way, 0, w_out, w_block(z, y, x, c), (z + way >= 0) & (z + way < nz))
    for src, dst, _ in weights:
        dst[d] = src[...]
    own_out = pl.ds(pl.multiple_of((s * dps + d) * part_out, part_out), part_out)
    w_g[own_out, :] = w_out[...]

    def norm(i, _):
        step = rows // 4
        band = pl.ds(pl.multiple_of(i * step, step), step)
        normed[band, :] = rms_scale(tokens[band, :].astype(jnp.float32), in_gain[...]).astype(jnp.bfloat16)
        return 0

    lax.fori_loop(0, 4, norm, 0)

    def relay(a):
        src, dst, split = weights[a]
        for dx in range(1, nx):
            origin = lax.rem(x - dx + nx, nx) * cores + c
            got = piece(dst.at[origin], split, y)
            links.arrive(("x", a, dx), got, at_dp(d))
            for dy in range(1, ny if split else 1):
                links.send(("y", a, dx, dy), got, got, at_sp(z * ny + lax.rem(y + dy, ny)))
            for dc, partner in partners:
                links.send(("cx", a, dx, dc), got, got, at_dp(partner))
        for dx in range(1, nx):
            origin = lax.rem(x - dx + nx, nx) * cores + c
            for dy in range(1, ny if split else 1):
                got = piece(dst.at[origin], split, lax.rem(y - dy + ny, ny))
                links.arrive(("y", a, dx, dy), got, at_dp(d))
                for dc, partner in partners:
                    links.send(("cy", a, dx, dy, dc), got, got, at_dp(partner))

    rope_key = jnp.dot(normed[:, : tokens.shape[1]], wrope[...], preferred_element_type=jnp.float32)
    kvr_g[s, :, kr:] = with_swapped(rope_key).astype(jnp.bfloat16)

    def settle(a):
        src, dst, split = weights[a]
        for dc, _ in partners:
            other = lax.rem(c - dc + cores, cores)
            links.arrive(("c", a, dc), dst.at[x * cores + other], at_dp(d))
            for dx in range(1, nx):
                origin = dst.at[lax.rem(x - dx + nx, nx) * cores + other]
                links.arrive(("cx", a, dx, dc), piece(origin, split, y), at_dp(d))
                for dy in range(1, ny if split else 1):
                    got = piece(origin, split, lax.rem(y - dy + ny, ny))
                    links.arrive(("cy", a, dx, dy, dc), got, at_dp(d))

    def down(gathered):
        part = gathered.shape[1]
        total = None
        for k in range(dps):
            term = jnp.dot(
                normed[:, k * part : (k + 1) * part], gathered[k], preferred_element_type=jnp.float32
            )
            total = term if total is None else total + term
        return total

    buffers = (kvr_g, q_g)

    def over_y(b, tag, slot, ok=None):
        block = buffers[b].at[slot]
        for dy in range(1, ny):
            links.send(("ly", b, tag, dy), block, block, at_sp(z * ny + lax.rem(y + dy, ny)), ok)

    def along_z(b, way, step, slot, ok):
        block = buffers[b].at[slot]
        links.send(("z", b, way, step), block, block, at_sp(jnp.clip(z + way, 0, nz - 1) * ny + y), ok)

    def launch(b):
        over_y(b, 0, s)
        for way in (1, -1):
            if nz > 1:
                along_z(b, way, 0, s, (z + way >= 0) & (z + way < nz))

    relay(0)
    settle(0)
    kvr_g[s, :, :kr] = rms_scale(down(wld_g), kv_lat_gain[...]).astype(jnp.bfloat16)
    launch(0)
    relay(1)
    settle(1)
    q_g[s] = rms_scale(down(wqd_g), q_lat_gain[...]).astype(jnp.bfloat16)
    launch(1)
    if nz > 1:
        w_z_step(0)
    for a in range(2, len(weights)):
        relay(a)
    for step in range(1, nz - 1):
        w_z_step(step)
    for k in range(nz):
        w_x(k, 0)

    for step in range(nz - 1):
        for b in range(2):
            for way in (1, -1):
                origin = z - way * (step + 1)
                ok = (origin >= 0) & (origin < nz)
                slot = jnp.clip(origin, 0, nz - 1) * ny + y
                links.arrive(("z", b, way, step), buffers[b].at[slot], at_sp(s), ok)
                if step < nz - 2:
                    along_z(b, way, step + 1, slot, ok & (z + way >= 0) & (z + way < nz))
                over_y(b, way * (step + 1), slot, ok)
    for k in range(nz):
        for dy in range(1, ny):
            block = w_block(lax.rem(z + k, nz), y, x, c)
            links.send(("wy", k, dy), block, block, at_sp(z * ny + lax.rem(y + dy, ny)))
    settle(2)
    settle(3)
    settle(4)
    wk_full = wku_g.reshape(dps * wku.shape[0], wku.shape[1])
    for k in range(dps):
        depth = wqu.shape[0]
        up = wqu_g[k].astype(jnp.float32)
        columns = []
        for h in range(heads):
            head = up[:, h * (wqu.shape[1] // heads) : (h + 1) * (wqu.shape[1] // heads)]
            columns += [head[:, :nope], with_swapped(head[:, nope:])]
        wq_s[k * depth : (k + 1) * depth, :] = jnp.concatenate(columns, axis=1).astype(jnp.bfloat16)
    wv_full = wvu_g.reshape(dps * wvu.shape[0], wvu.shape[1])
    wvt[...] = jnp.transpose(wv_full[...].astype(jnp.float32)).astype(jnp.bfloat16)
    gq, gk = q_gain[:, :nope], k_gain[:, :nope]
    gq2, gk2 = with_swapped(q_gain[:, nope:]), with_swapped(k_gain[:, nope:])
    def project(j, _):
        i = lax.rem(j, nz) * ny + lax.rem(y + lax.div(j, nz), ny)
        project_block(
            i, rows, heads, nope, vd, q_g[i], kvr_g[i, :, :kr], kvr_g[i, :, kr:],
            wq_s, wk_full, wvt, gq, gk, gq2, gk2, table, q_s, k_s, v_s,
        )
        return 0

    lax.fori_loop(0, nz, project, 0)
    for b in range(2):
        for tag in range(1 - nz, nz):
            zz = z - tag
            ok = None if tag == 0 else (zz >= 0) & (zz < nz)
            for dy in range(1, ny):
                slot = jnp.clip(zz, 0, nz - 1) * ny + lax.rem(y - dy + ny, ny)
                links.arrive(("ly", b, tag, dy), buffers[b].at[slot], at_sp(s), ok)
    lax.fori_loop(nz, seqs, project, 0)

    def hand_over(qb):
        return pltpu.make_async_remote_copy(
            src_ref=att_s.at[qb], dst_ref=heads_g.at[s], send_sem=a2a_send.at[qb],
            recv_sem=a2a_recv.at[s], device_id=at_sp(qb), device_id_type=MESH,
        )

    def attend(i, _):
        qb = lax.rem(s + 1 + i, seqs)
        att_s[qb] = attend_block(qb, rows, chunk, heads, vd, scale, q_s, k_s, v_s)

        @pl.when(i < seqs - 1)
        def _():
            hand_over(qb).start()

        return 0

    lax.fori_loop(0, seqs // 2, attend, 0)
    for k in range(nz):
        for dy in range(1, ny):
            block = w_block(lax.rem(z + k, nz), lax.rem(y - dy + ny, ny), x, c)
            links.arrive(("wy", k, dy), block, at_sp(s))
            w_x(k, dy)
    for k in range(nz):
        w_x_arrive(k, 0)
    lax.fori_loop(seqs // 2, seqs, attend, 0)
    for k in range(nz):
        for dy in range(1, ny):
            w_x_arrive(k, dy)
    heads_g[s] = att_s[s]
    for k in range(1, seqs):
        origin = lax.rem(s + k, seqs)
        pltpu.make_async_remote_copy(
            src_ref=att_s.at[origin], dst_ref=heads_g.at[origin], send_sem=a2a_send.at[origin],
            recv_sem=a2a_recv.at[origin], device_id=at_sp(origin), device_id_type=MESH,
        ).wait()
    width = heads * vd
    square = jnp.zeros((rows, 1), jnp.float32)
    for k in range(seqs):
        block = heads_g[k].astype(jnp.float32)
        square = square + jnp.sum(block * block, axis=-1, keepdims=True)
    r = lax.rsqrt(square * (1.0 / (seqs * width)) + EPS)
    for k in range(seqs):
        cols = slice(k * width, (k + 1) * width)
        normed[:, cols] = (heads_g[k].astype(jnp.float32) * r * out_gain[:, cols]).astype(jnp.bfloat16)
    for k in range(nz):
        for dy in range(ny):
            for dx in range(nx):
                for dc, _ in partners:
                    block = w_block(
                        lax.rem(z + k, nz), lax.rem(y - dy + ny, ny), lax.rem(x - dx + nx, nx),
                        lax.rem(c - dc + cores, cores),
                    )
                    links.arrive(("wc", k, dy, dx, dc), block, at_dp(d))
    tile = 256 if out.shape[1] % 256 == 0 else out.shape[1]

    def project_out(i, _):
        cols = pl.ds(pl.multiple_of(i * tile, tile), tile)
        out[:, cols] = jnp.dot(normed[...], w_g[:, cols], preferred_element_type=jnp.float32).astype(out.dtype)
        return 0

    lax.fori_loop(0, out.shape[1] // tile, project_out, 0)
    links.drain()


def per_device(
    tokens, in_gain, w_query_down, w_latent_down, w_rope_key, query_latent_gain, latent_gain,
    w_query_up, w_key_up, w_value_up, query_gain, key_gain, out_gain, w_out,
):
    seqs, dps = lax.axis_size("sp"), lax.axis_size("dp")
    cores = 2 if dps % 2 == 0 else 1
    nx = dps // cores
    ny = nx if seqs % nx == 0 else 1
    nz = seqs // ny
    heads = HEADS // seqs
    own_rows = tokens.shape[1]
    length = own_rows * seqs
    rope = w_rope_key.shape[1]
    nope = w_key_up.shape[1] // heads
    vd = w_value_up.shape[1] // heads
    wide = nope + 2 * rope
    chunk = min(2 * own_rows, length)
    sems = sem_count(nx, ny, nz, cores)
    b16 = jnp.bfloat16

    def gathered(w):
        return pltpu.VMEM((dps,) + w.shape, b16)

    result = pl.pallas_call(
        functools.partial(
            layer_kernel, (nx, ny, nz, cores), chunk, heads, nope, vd, float(nope + rope) ** -0.5
        ),
        out_shape=jax.ShapeDtypeStruct((own_rows, w_out.shape[1]), b16),
        in_specs=[pl.BlockSpec(memory_space=pltpu.VMEM)] * 15,
        out_specs=pl.BlockSpec(memory_space=pltpu.VMEM),
        scratch_shapes=[
            pltpu.VMEM((own_rows, max(tokens.shape[2], w_out.shape[0] * seqs * dps)), b16),
            gathered(w_query_down), gathered(w_latent_down), gathered(w_query_up), gathered(w_key_up), gathered(w_value_up),
            pltpu.VMEM((w_out.shape[0] * seqs * dps, w_out.shape[1]), b16),
            pltpu.VMEM((w_query_down.shape[1], heads * wide), b16),
            pltpu.VMEM((heads * vd, w_latent_down.shape[1]), b16),
            pltpu.VMEM((seqs, own_rows, w_latent_down.shape[1] + 2 * rope), b16),
            pltpu.VMEM((seqs, own_rows, w_query_down.shape[1]), b16),
            pltpu.VMEM((heads, length, wide), b16),
            pltpu.VMEM((heads, length, wide), b16),
            pltpu.VMEM((heads * vd, length), b16),
            pltpu.VMEM((seqs, own_rows, heads * vd), b16),
            pltpu.VMEM((seqs, own_rows, heads * vd), b16),
            pltpu.SemaphoreType.DMA((sems,)),
            pltpu.SemaphoreType.DMA((sems,)),
            pltpu.SemaphoreType.DMA((seqs,)),
            pltpu.SemaphoreType.DMA((seqs,)),
        ],
        compiler_params=pltpu.CompilerParams(
            vmem_limit_bytes=56 * 1024 * 1024, collective_id=0, has_side_effects=True
        ),
        cost_estimate=pl.CostEstimate(flops=60 * 10**9, bytes_accessed=10**8, transcendentals=5 * 10**6),
    )(
        tokens.reshape(own_rows, tokens.shape[2]), in_gain[None], w_query_down, w_latent_down, w_rope_key,
        query_latent_gain[None], latent_gain[None], w_query_up, w_key_up, w_value_up,
        query_gain[None], key_gain[None], jnp.asarray(rotation_table(length, rope)), out_gain[None], w_out,
    )
    return result.reshape(1, own_rows, w_out.shape[1])


def solution(mesh):
    in_specs = (
        P("dp", "sp", None), P(), P("dp", None), P("dp", None), P(), P(), P(),
        P("dp", "sp"), P("dp", "sp"), P("dp", "sp"), P(), P(), P(), P(("sp", "dp"), None),
    )
    return jax.shard_map(
        per_device, mesh=mesh, in_specs=in_specs, out_specs=P("dp", "sp", None), check_vma=False
    )
```
